32 devices in a mesh: sp: 8 (over z, y), tp: 4 (over x, core).
Axes of the slice: x: 2, y: 2, z: 4, core: 2. Of those that a mesh axis runs over, the one named last changes fastest.
Arguments:
- residual: bfloat16 [4, 768, 2048], P('tp', 'sp'), may hold values from -3 to 3
- query_nope: bfloat16 [4, 768, 1024], P('tp', 'sp'), may hold values from -9 to 9
- query_rope: bfloat16 [4, 768, 512], P('tp', 'sp'), may hold values from -48 to 48
- latent: bfloat16 [4, 768, 128], P('tp', 'sp'), may hold values from -6 to 6
- rope_key: bfloat16 [4, 768, 32], P('tp', 'sp'), may hold values from -48 to 48
- latent_gain: float32 [128], replicated, may hold values from 0.1 to 1.9
- up_key: bfloat16 [128, 1024], replicated, may hold values from -1 to 1
- up_value: bfloat16 [128, 1024], replicated, may hold values from -0.5 to 0.5
- out_weight: bfloat16 [1024, 2048], replicated, may hold values from -0.375 to 0.375
- ffn_gain: float32 [2048], replicated, may hold values from 0.1 to 1.9
- routes: int32 [4, 768, 2], P(None, 'sp'), may hold values from 0 to 7, all different within a row; in each aligned block of 96 rows (0 to 95, 96 to 191, ..., all dimensions but the last counted through in order) at most 30 rows name the same one
- route_weight: float32 [4, 768, 2], P('tp', 'sp'), may hold values from 0.1 to 1
- gate_weight: bfloat16 [8, 2048, 1024], P('sp', None, 'tp'), may hold values from -1.5 to 1.5
- up_weight: bfloat16 [8, 2048, 1024], P('sp', None, 'tp'), may hold values from -1.5 to 1.5
- down_weight: bfloat16 [8, 1024, 2048], P('sp', 'tp'), may hold values from -0.046875 to 0.046875
Outputs:
- updated: bfloat16 [4, 768, 2048], P('tp', 'sp')
The draws below stay inside these ranges and needn't reach their ends.
Inputs may be any that keep to these rules, and one draw needn't show every extreme that they name: `routes`: each row names 2 different experts. In each aligned block of 96 rows (one sequence's rows of one device) no expert is named by more than 30 rows, a bound that some block reaches.
All inputs are finite; a program needn't handle non-finite values.
Results may differ from the reference program's by a relative error of at most 0.017.
Values may be sent and summed in bfloat16 or wider, within the bound.
A program may use at most 64 MiB of HBM per device.

```python
import math
import jax
import jax.numpy as jnp
import numpy as np
from jax import lax

D = 2048
HEADS = 16
NOPE = 64
ROPE = 32
VDIM = 64
LATENT = 128
FF = 1024
TOPK = 2
TOK_DEV = 96
SEQS = 4
LENGTH = 768
EXPERTS = 8
FF_BLOCK = 256
MOST = 30
N_SP = 8
N_TP = 4


def rope_pair(key):
    base = jax.random.fold_in(key, 7)
    shape_keys = (SEQS, LENGTH, ROPE)
    shape_queries = (SEQS, LENGTH, HEADS, ROPE)
    keys = jax.random.normal(jax.random.fold_in(base, 1), shape_keys, jnp.float32) * 1.5
    queries = jax.random.normal(jax.random.fold_in(base, 2), shape_queries, jnp.float32) * 1.5
    return (keys, queries.reshape(SEQS, LENGTH, HEADS * ROPE))


def expert_matrix(key, salt):
    base = jax.random.fold_in(key, salt)
    values = jax.random.normal(jax.random.fold_in(base, 1), (EXPERTS, D, FF), jnp.float32)
    columns = jnp.exp(jax.random.uniform(jax.random.fold_in(base, 2), (EXPERTS, 1, FF), jnp.float32, math.log(0.5), math.log(6.0)))
    return jnp.clip(values * columns * D ** (-0.5), -1.5, 1.5)


def draw_query_rope(key, part):
    return rope_pair(key)[1].astype(jnp.bfloat16)


def draw_rope_key(key, part):
    return rope_pair(key)[0].astype(jnp.bfloat16)


def draw_gate_weight(key, part):
    return expert_matrix(key, 101).astype(jnp.bfloat16)


def draw_up_weight(key, part):
    return expert_matrix(key, 202).astype(jnp.bfloat16)


def level_of(stream_key, shape, shards, low, high):
    level, own = 1.0, jax.random.fold_in(stream_key, 6)
    for dim, shards_of in shards:
        steps = jnp.exp(jax.random.uniform(jax.random.fold_in(own, dim), (shards_of,), jnp.float32, low / len(shards), high / len(shards)))
        level = level * jnp.repeat(steps, shape[dim] // shards_of).reshape([-1 if axis == dim else 1 for axis in range(len(shape))])
    return level


def shared_out(own_key, own, number, rows, amount, top, limit, lean):
    order = jax.random.permutation(own_key, amount)
    packed, ordinary = load_shares(amount, rows * top, limit, lean, True), load_shares(amount, rows * top, limit, lean, False)
    places = jnp.arange(amount)

    def named(tallies, offset_by):
        used = int((tallies > 0).sum())
        fixed = max(1, used // 4)
        passed = fixed + (places - fixed + offset_by * (used - fixed)) % max(1, amount - fixed)
        return jnp.zeros((amount,), jnp.int32).at[order[jnp.where(places < fixed, places, passed)]].set(jnp.asarray(tallies, jnp.int32))

    tallies = jnp.where(number % 4 == 0, named(packed, number // 4), named(ordinary, number - number // 4 - 1))
    mixed = jax.random.permutation(jax.random.fold_in(own, 3), amount)
    giver, sink = mixed[0:amount // 2 * 2:2], mixed[1:amount // 2 * 2:2]
    room = jnp.minimum(tallies[giver] - 1, limit - tallies[sink]) // 2
    room = jnp.where((giver == order[0]) | (sink == order[0]) | (tallies[sink] == 0), 0, jnp.maximum(room, 0))
    passed = jax.random.randint(jax.random.fold_in(own, 4), (amount // 2,), 0, 1 << 20) % (room + 1)
    tallies = tallies.at[giver].add(-passed).at[sink].add(passed)
    members = jnp.searchsorted(jnp.cumsum(tallies), jnp.arange(rows * top), side="right").astype(jnp.int32)
    grid = members.reshape(top, rows).T
    grid = grid[jax.random.permutation(jax.random.fold_in(own, 1), rows)]
    offset_by = jax.random.randint(jax.random.fold_in(own, 2), (rows, 1), 0, top)
    return jnp.take_along_axis(grid, (jnp.arange(top)[None, :] + offset_by) % top, axis=1)


def load_shares(count, total, reach, skew, full):
    portions = [(1 << 20) // math.isqrt(standing ** skew) + 1 for standing in range(1, count + 1)]
    largest = reach if full else min(reach, max(-(-total // count), total * portions[0] // sum(portions)))
    least = 1 if total - largest >= count - 1 else 0
    given, rest = [largest] + [least] * (count - 1), total - largest - least * (count - 1)
    while rest > 0:
        candidates = [i for i in range(1, count) if given[i] < largest] or [i for i in range(1, count) if given[i] < reach]
        whole, budget = sum([portions[i] for i in candidates]), rest
        for i in candidates:
            addition = min(reach - given[i], max(1, budget * portions[i] // whole), rest)
            given[i] = given[i] + addition
            rest = rest - addition
    return np.array(given)


def bell_draw(own_key, dims, spread, most, shards=(), held_as=jnp.bfloat16):
    loudness = level_of(own_key, dims, shards, -0.22, 0.18) if shards else 1.0
    values = jax.random.normal(own_key, dims, jnp.float32) * spread * loudness
    return jnp.minimum(jnp.maximum(values, -most), most).astype(held_as)


def setup_inputs(seed: int = 0) -> dict:
    key_list = jax.random.split(jax.random.key(seed), 16)
    residual = bell_draw(key_list[0], (SEQS, LENGTH, D), 0.5, 3.0, ((0, 4), (1, 8)))
    query_nope = bell_draw(key_list[1], (SEQS, LENGTH, HEADS * NOPE), 1.5, 9.0, ((0, 4), (1, 8)))
    query_rope = draw_query_rope(jax.random.fold_in(key_list[15], 71), 0)
    latent = bell_draw(key_list[3], (SEQS, LENGTH, LATENT), 1.0, 6.0, ((0, 4), (1, 8)))
    rope_key = draw_rope_key(jax.random.fold_in(key_list[15], 71), 0)
    latent_gain = jnp.clip(1.0 + 0.18 * jax.random.normal(key_list[5], (LATENT,), jnp.float32), 0.1, 1.9)
    up_key = bell_draw(key_list[6], (LATENT, HEADS * NOPE), (LATENT // 3) ** -0.5, 1.0)
    up_value = bell_draw(key_list[7], (LATENT, HEADS * VDIM), LATENT ** -0.5, 0.5)
    out_weight = bell_draw(key_list[8], (HEADS * VDIM, D), (HEADS * VDIM // 4) ** -0.5, 0.375)
    ffn_gain = jnp.clip(1.0 + 0.18 * jax.random.normal(key_list[9], (D,), jnp.float32), 0.1, 1.9)
    routes_keys = jax.random.split(jax.random.fold_in(key_list[10], 1), SEQS * LENGTH // TOK_DEV)
    routes_turns = jax.random.permutation(jax.random.fold_in(key_list[10], 3), SEQS * LENGTH // TOK_DEV)
    routes = jax.vmap(lambda own, number: shared_out(jax.random.fold_in(key_list[10], 2), own, number, TOK_DEV, EXPERTS, TOPK, MOST, 0))(routes_keys, routes_turns).reshape((SEQS, LENGTH, TOPK))
    route_weight = jnp.clip(jnp.exp(math.log(1.0) - 2.3025851 * jax.random.uniform(key_list[11], (SEQS, LENGTH, TOPK), jnp.float32) ** level_of(key_list[11], (SEQS, LENGTH, TOPK), ((0, 4), (1, 8)), -0.2, 0.2)), 0.1, 1.0)
    gate_weight = draw_gate_weight(jax.random.fold_in(key_list[15], 71), 0)
    up_weight = draw_up_weight(jax.random.fold_in(key_list[15], 71), 0)
    down_weight = bell_draw(key_list[14], (EXPERTS, FF, D), (FF * 16) ** -0.5, 0.046875, ((0, 8), (1, 4)))
    return dict(residual=residual, query_nope=query_nope, query_rope=query_rope, latent=latent, rope_key=rope_key, latent_gain=latent_gain, up_key=up_key, up_value=up_value, out_weight=out_weight, ffn_gain=ffn_gain, routes=routes, route_weight=route_weight, gate_weight=gate_weight, up_weight=up_weight, down_weight=down_weight)


EPS = 1e-06
ROPE_BASE = 10000.0
CLAMP = 7.0
ALPHA = 1.702

def rotate(values, positions, width):
    half = width // 2
    inverse = ROPE_BASE ** (-jnp.arange(half, dtype=jnp.float32) * 2.0 / width)
    angle = positions.astype(jnp.float32)[:, None] * inverse[None, :]
    cosine = jnp.cos(angle)[:, None, :]
    sine = jnp.sin(angle)[:, None, :]
    first = values[..., :half]
    second = values[..., half:]
    return jnp.concatenate([first * cosine - second * sine, first * sine + second * cosine], axis=-1)

def rms_scaled(values, gain):
    return values * lax.rsqrt(lax.optimization_barrier(jnp.mean(values * values, axis=-1, keepdims=True)) + EPS) * gain

def reference(residual, query_nope, query_rope, latent, rope_key, latent_gain, up_key, up_value, out_weight, ffn_gain, routes, route_weight, gate_weight, up_weight, down_weight):
    sequences, length, width = residual.shape
    positions = jnp.arange(length, dtype=jnp.int32)
    factor = (NOPE + ROPE) ** (-0.5)
    normed = rms_scaled(latent.astype(jnp.float32), latent_gain).astype(jnp.bfloat16)
    flat_latent = normed.reshape(-1, LATENT)
    key_part = jnp.dot(flat_latent, up_key, preferred_element_type=jnp.float32).astype(jnp.bfloat16)
    key_part = key_part.reshape(sequences, length, HEADS, NOPE)
    value_part = jnp.dot(flat_latent, up_value, preferred_element_type=jnp.float32).astype(jnp.bfloat16)
    value_part = value_part.reshape(sequences, length, HEADS, VDIM)
    key_turned = rotate(rope_key.astype(jnp.float32)[:, :, None, :], positions, ROPE)[:, :, 0, :].astype(jnp.bfloat16)
    query_turned = rotate(query_rope.astype(jnp.float32).reshape(sequences, length, HEADS, ROPE), positions, ROPE).astype(jnp.bfloat16)
    query_plain = query_nope.reshape(sequences, length, HEADS, NOPE)
    span = math.gcd(length, 256)
    count = length // span

    def one_sequence(items):
        plain, turned, keys, turned_keys, values = items
        keys_wide = keys.astype(jnp.float32)
        turned_wide = turned_keys.astype(jnp.float32)
        values_wide = values.astype(jnp.float32)

        def one_block(pair):
            scores = (jnp.einsum('qhd,khd->hqk', pair[0].astype(jnp.float32), keys_wide) + jnp.einsum('qhd,kd->hqk', pair[1].astype(jnp.float32), turned_wide)) * factor
            peak = lax.optimization_barrier(jnp.max(scores, axis=-1, keepdims=True))
            weights = jnp.exp(scores - peak)
            total = lax.optimization_barrier(jnp.sum(weights, axis=-1))
            rounded = lax.optimization_barrier(weights.astype(jnp.bfloat16)).astype(jnp.float32)
            mixed = jnp.einsum('hqk,khd->qhd', rounded, values_wide)
            return (mixed / jnp.transpose(total)[:, :, None]).astype(jnp.bfloat16)
        blocks = lax.map(one_block, (plain.reshape(count, span, HEADS, NOPE), turned.reshape(count, span, HEADS, ROPE)))
        return blocks.reshape(length, HEADS * VDIM)
    attended = lax.map(one_sequence, (query_plain, query_turned, key_part, key_turned, value_part))
    projected = jnp.dot(attended.reshape(-1, HEADS * VDIM), out_weight, preferred_element_type=jnp.float32)
    middle = (residual.reshape(-1, width).astype(jnp.float32) + projected).astype(jnp.bfloat16)
    middle_wide = lax.optimization_barrier(middle).astype(jnp.float32)
    normal_rows = rms_scaled(middle_wide, ffn_gain).astype(jnp.bfloat16)
    total_rows = sequences * length
    flat_picks = routes.reshape(-1)
    flat_weights = route_weight.reshape(-1)
    owner = jnp.arange(total_rows * TOPK, dtype=jnp.int32) // TOPK
    capacity = sequences * N_SP * MOST
    padded = jnp.concatenate([normal_rows, jnp.zeros((1, width), jnp.bfloat16)], axis=0)

    def one_expert(accum, items):
        gate_w, up_w, down_w, index = items
        hit = flat_picks == index
        rank = jnp.cumsum(hit.astype(jnp.int32)) - 1
        slot = jnp.where(hit, rank, capacity).astype(jnp.int32)
        source = jnp.full((capacity + 1,), total_rows, jnp.int32).at[slot].set(owner)[:capacity]
        scale_rows = jnp.zeros((capacity + 1,), jnp.float32).at[slot].set(flat_weights)[:capacity]
        rows = padded[source]
        gate = jnp.minimum(jnp.dot(rows, gate_w, preferred_element_type=jnp.float32), CLAMP)
        lift = jnp.clip(jnp.dot(rows, up_w, preferred_element_type=jnp.float32), -CLAMP, CLAMP)
        active = (gate * jax.nn.sigmoid(ALPHA * gate) * (lift + 1.0)).astype(jnp.bfloat16)
        parts = jnp.einsum('rjf,jfd->jrd', active.reshape(capacity, N_TP, FF_BLOCK).astype(jnp.float32), down_w.reshape(N_TP, FF_BLOCK, width).astype(jnp.float32))
        output = lax.optimization_barrier(jnp.sum(lax.optimization_barrier(parts.astype(jnp.bfloat16)).astype(jnp.float32), axis=0))
        output = output.astype(jnp.bfloat16)
        accum = accum.at[source].add(output.astype(jnp.float32) * scale_rows[:, None])
        return (accum, None)
    accum, _ = lax.scan(one_expert, jnp.zeros((total_rows + 1, width), jnp.float32), (gate_weight, up_weight, down_weight, jnp.arange(EXPERTS, dtype=jnp.int32)))
    updated = (middle_wide + accum[:total_rows]).astype(jnp.bfloat16)
    return updated.reshape(sequences, length, width)
```

```python
import functools

import jax
import jax.numpy as jnp
from jax import lax
from jax.experimental import pallas as pl
from jax.experimental.pallas import tpu as pltpu
from jax.sharding import PartitionSpec as P

HEADS = 16
NOPE = 64
ROPE = 32
VDIM = 64
LATENT = 128
TOPK = 2
LANES = 128

EPS = 1e-06
ROPE_BASE = 10000.0
CLAMP = 7.0
ALPHA = 1.702
MESH = pl.DeviceIdType.MESH
VM = pl.BlockSpec(memory_space=pltpu.VMEM)
F32 = jnp.float32
BF16 = jnp.bfloat16


def swapped(x):
    lane = lax.broadcasted_iota(jnp.int32, x.shape, 1)
    half = ROPE // 2
    return jnp.where(
        lane % ROPE < half, pltpu.roll(x, x.shape[1] - half, 1), pltpu.roll(x, half, 1)
    )


def prep_kernel(lat_ref, gain_ref, rk_ref, cos_ref, sin_ref, blk_ref):
    lat = lat_ref[...].astype(F32)
    mean = jnp.mean(lat * lat, axis=-1, keepdims=True)
    blk_ref[:, :LATENT] = (lat * lax.rsqrt(mean + EPS) * gain_ref[...]).astype(BF16)
    rk = rk_ref[...].astype(F32)
    blk_ref[:, LATENT:] = (rk * cos_ref[...] + swapped(rk) * sin_ref[...]).astype(BF16)


def place(picks_ref, experts, slots, tokens):
    expert = lax.broadcasted_iota(jnp.int32, (experts, tokens), 0)
    hots = [(expert == picks_ref[k : k + 1, :]).astype(F32) for k in range(TOPK)]
    earlier = (
        lax.broadcasted_iota(jnp.int32, (tokens, tokens), 0)
        < lax.broadcasted_iota(jnp.int32, (tokens, tokens), 1)
    ).astype(F32)
    rank = jnp.dot(sum(hots), earlier, preferred_element_type=F32)
    where = rank + (expert * slots).astype(F32)
    slot = lax.broadcasted_iota(jnp.int32, (experts * slots, tokens), 0).astype(F32)
    return [
        (slot == jnp.sum(hot * where, axis=0, keepdims=True)).astype(F32) for hot in hots
    ]


def attend_kernel(
    n, slots,
    blk_ref, qn_ref, qr_ref, cos_ref, sin_ref, upk_ref, upv_ref, ow_ref, res_ref, gain_ref,
    picks_ref, mid_ref, out_ref, rows, qrot, att, norm, send_sem, recv_sem,
):
    tokens = blk_ref.shape[0]
    width = res_ref.shape[1]
    me = lax.axis_index("sp")
    barrier = pltpu.get_barrier_semaphore()
    for d in range(1, n):
        pl.semaphore_signal(
            barrier, inc=1, device_id={"sp": lax.rem(me + d, n)}, device_id_type=MESH
        )
    pl.semaphore_wait(barrier, n - 1)
    copies = []
    for d in range(1, n):
        copy = pltpu.make_async_remote_copy(
            src_ref=blk_ref,
            dst_ref=rows.at[pl.ds(d * tokens, tokens)],
            send_sem=send_sem.at[d],
            recv_sem=recv_sem.at[d],
            device_id={"sp": lax.rem(me + d, n)},
            device_id_type=MESH,
        )
        copy.start()
        copies.append(copy)
    rows[:tokens, :] = blk_ref[...]
    for g in range(HEADS * ROPE // LANES):
        x = qr_ref[:, g * LANES : (g + 1) * LANES].astype(F32)
        qrot[:, g * LANES : (g + 1) * LANES] = (
            x * cos_ref[...] + swapped(x) * sin_ref[...]
        ).astype(BF16)
    factor = (NOPE + ROPE) ** (-0.5)
    lane = lax.broadcasted_iota(jnp.int32, (tokens, LANES), 1)
    low = lane < NOPE
    lowb = low.astype(F32).astype(BF16)
    highb = (lane >= NOPE).astype(F32).astype(BF16)
    ropeb = [(lane // ROPE == k).astype(F32).astype(BF16) for k in range(LANES // ROPE)]
    for copy in copies:
        copy.wait()

    def group(g, carry):
        turned = qrot[:, pl.ds(pl.multiple_of(g * LANES, LANES), LANES)]
        for q in range(2):
            lanes = pl.ds(pl.multiple_of((g * 2 + q) * LANES, LANES), LANES)
            lat = rows[:, :LATENT]
            keys = jnp.dot(lat, upk_ref[:, lanes], preferred_element_type=F32).astype(BF16)
            vals = jnp.dot(lat, upv_ref[:, lanes], preferred_element_type=F32).astype(BF16)
            keys = jnp.concatenate([keys, rows[:, LATENT:]], axis=1)
            plain = qn_ref[:, lanes]
            first = jnp.concatenate([plain * lowb, turned * ropeb[2 * q]], axis=1)
            second = jnp.concatenate([plain * highb, turned * ropeb[2 * q + 1]], axis=1)
            query = jnp.concatenate([first, second], axis=0)
            scores = lax.dot_general(
                query, keys, (((1,), (1,)), ((), ())), preferred_element_type=F32
            ) * factor
            weights = jnp.exp(scores - jnp.max(scores, axis=-1, keepdims=True))
            total = jnp.sum(weights, axis=-1, keepdims=True)
            mixed = jnp.dot(weights.astype(BF16), vals, preferred_element_type=F32) / total
            att[:, lanes] = jnp.where(low, mixed[:tokens], mixed[tokens:]).astype(BF16)
        return carry

    lax.fori_loop(0, HEADS * ROPE // LANES, group, 0)
    step = 512

    def project(c, square):
        cols = pl.ds(pl.multiple_of(c * step, step), step)
        product = jnp.dot(att[...], ow_ref[:, cols], preferred_element_type=F32)
        middle = (res_ref[:, cols].astype(F32) + product).astype(BF16)
        mid_ref[:, cols] = middle
        wide = middle.astype(F32)
        return square + jnp.sum(wide * wide, axis=-1, keepdims=True)

    square = lax.fori_loop(0, width // step, project, jnp.zeros((tokens, 1), F32))
    scale = lax.rsqrt(square / width + EPS)
    norm[...] = (mid_ref[...].astype(F32) * scale * gain_ref[...]).astype(BF16)
    packer = sum(place(picks_ref, n, slots, tokens)).astype(BF16)

    def pack(c, carry):
        cols = pl.ds(pl.multiple_of(c * step, step), step)
        out_ref[:, cols] = jnp.dot(packer, norm[:, cols], preferred_element_type=F32).astype(BF16)
        return carry

    lax.fori_loop(0, width // step, pack, 0)


def combine_kernel(n, slots, mid_ref, back_ref, picks_ref, weight_ref, out_ref):
    tokens, width = mid_ref.shape
    spots = place(picks_ref, n, slots, tokens)
    high = low = 0.0
    for k in range(TOPK):
        weight = weight_ref[k : k + 1, :]
        coarse = weight.astype(BF16).astype(F32)
        high = high + spots[k] * coarse
        low = low + spots[k] * (weight - coarse)
    high = high.astype(BF16)
    low = low.astype(BF16)
    dims = (((0,), (0,)), ((), ()))
    step = 512

    def chunk(c, carry):
        cols = pl.ds(pl.multiple_of(c * step, step), step)
        back = back_ref[:, cols]
        added = lax.dot_general(high, back, dims, preferred_element_type=F32)
        added = added + lax.dot_general(low, back, dims, preferred_element_type=F32)
        out_ref[:, cols] = (mid_ref[:, cols].astype(F32) + added).astype(BF16)
        return carry

    lax.fori_loop(0, width // step, chunk, 0)


def expert_term(rows, gate_w, up_w, down_w):
    gate = jnp.minimum(jnp.dot(rows, gate_w, preferred_element_type=F32), CLAMP)
    lift = jnp.clip(jnp.dot(rows, up_w, preferred_element_type=F32), -CLAMP, CLAMP)
    active = (gate * jax.nn.sigmoid(ALPHA * gate) * (lift + 1.0)).astype(BF16)
    return jnp.dot(active, down_w, preferred_element_type=F32)


def local(
    residual, query_nope, query_rope, latent, rope_key, latent_gain, up_key, up_value,
    out_weight, ffn_gain, routes, route_weight, gate_weight, up_weight, down_weight,
):
    tokens, width = residual.shape[1:]
    n = lax.axis_size("sp")
    slots = min(tokens, max(2, 5 * tokens * TOPK // (4 * n)))
    slots = -(-slots // 16) * 16
    positions = lax.axis_index("sp") * tokens + jnp.arange(tokens, dtype=jnp.int32)
    lane = jnp.arange(LANES, dtype=jnp.int32)
    half = ROPE // 2
    inverse = ROPE_BASE ** (-(lane % half).astype(F32) * 2.0 / ROPE)
    angle = positions.astype(F32)[:, None] * inverse[None, :]
    cosine = jnp.cos(angle)
    sine = jnp.sin(angle) * jnp.where(lane % ROPE < half, -1.0, 1.0)[None, :]
    blk = pl.pallas_call(
        prep_kernel,
        out_shape=jax.ShapeDtypeStruct((tokens, 2 * LANES), BF16),
        in_specs=[VM] * 5,
        out_specs=VM,
    )(latent[0], latent_gain[None, :], jnp.tile(rope_key[0], (1, LANES // ROPE)), cosine, sine)
    picks = lax.dynamic_index_in_dim(
        jnp.transpose(routes, (0, 2, 1)), lax.axis_index("tp"), 0, keepdims=False
    )
    middle, outgoing = pl.pallas_call(
        functools.partial(attend_kernel, n, slots),
        out_shape=(
            jax.ShapeDtypeStruct((tokens, width), BF16),
            jax.ShapeDtypeStruct((n * slots, width), BF16),
        ),
        in_specs=[VM] * 11,
        out_specs=(VM, VM),
        scratch_shapes=[
            pltpu.VMEM((n * tokens, 2 * LANES), BF16),
            pltpu.VMEM((tokens, HEADS * ROPE), BF16),
            pltpu.VMEM((tokens, HEADS * VDIM), BF16),
            pltpu.VMEM((tokens, width), BF16),
            pltpu.SemaphoreType.DMA((n,)),
            pltpu.SemaphoreType.DMA((n,)),
        ],
        compiler_params=pltpu.CompilerParams(
            collective_id=0, has_side_effects=True, vmem_limit_bytes=60 * 2**20
        ),
    )(
        blk, query_nope[0], query_rope[0], cosine, sine, up_key, up_value, out_weight,
        residual[0], ffn_gain[None, :], picks,
    )
    arrived = lax.all_to_all(
        outgoing.reshape(1, n, slots, width), "sp", split_axis=1, concat_axis=1, tiled=True
    ).reshape(n * slots, width)
    gathered = lax.all_gather(arrived, "tp", axis=0, tiled=True)
    terms = expert_term(gathered, gate_weight[0], up_weight[0], down_weight[0])
    mine = lax.psum_scatter(terms.astype(BF16), "tp", scatter_dimension=0, tiled=True)
    returned = lax.all_to_all(
        mine.reshape(1, n, slots, width), "sp", split_axis=1, concat_axis=1, tiled=True
    )
    updated = pl.pallas_call(
        functools.partial(combine_kernel, n, slots),
        out_shape=jax.ShapeDtypeStruct((tokens, width), BF16),
        in_specs=[VM] * 4,
        out_specs=VM,
    )(middle, returned.reshape(n * slots, width), picks, jnp.transpose(route_weight[0], (1, 0)))
    return updated[None]


def solution(mesh):
    in_specs = (
        P("tp", "sp", None),
        P("tp", "sp", None),
        P("tp", "sp", None),
        P("tp", "sp", None),
        P("tp", "sp", None),
        P(),
        P(),
        P(),
        P(),
        P(),
        P(None, "sp", None),
        P("tp", "sp", None),
        P("sp", None, "tp"),
        P("sp", None, "tp"),
        P("sp", "tp", None),
    )
    out_specs = P("tp", "sp", None)
    return jax.shard_map(local, mesh=mesh, in_specs=in_specs, out_specs=out_specs, check_vma=False)
```

```python
import functools

import jax
import jax.numpy as jnp
from jax import lax
from jax.experimental import pallas as pl
from jax.experimental.pallas import tpu as pltpu
from jax.sharding import PartitionSpec as P

HEADS = 16
NOPE = 64
ROPE = 32
VDIM = 64
LATENT = 128
TOPK = 2
LANES = 128

EPS = 1e-06
ROPE_BASE = 10000.0
CLAMP = 7.0
ALPHA = 1.702
MESH = pl.DeviceIdType.MESH
VM = pl.BlockSpec(memory_space=pltpu.VMEM)
F32 = jnp.float32
BF16 = jnp.bfloat16


def swapped(x):
    lane = lax.broadcasted_iota(jnp.int32, x.shape, 1)
    half = ROPE // 2
    return jnp.where(
        lane % ROPE < half, pltpu.roll(x, x.shape[1] - half, 1), pltpu.roll(x, half, 1)
    )


def prep_kernel(lat_ref, gain_ref, rk_ref, cos_ref, sin_ref, blk_ref):
    lat = lat_ref[...].astype(F32)
    mean = jnp.mean(lat * lat, axis=-1, keepdims=True)
    blk_ref[:, :LATENT] = (lat * lax.rsqrt(mean + EPS) * gain_ref[...]).astype(BF16)
    rk = rk_ref[...].astype(F32)
    blk_ref[:, LATENT:] = (rk * cos_ref[...] + swapped(rk) * sin_ref[...]).astype(BF16)


def place(picks_ref, experts, slots, tokens):
    expert = lax.broadcasted_iota(jnp.int32, (experts, tokens), 0)
    hots = [(expert == picks_ref[k : k + 1, :]).astype(F32) for k in range(TOPK)]
    earlier = (
        lax.broadcasted_iota(jnp.int32, (tokens, tokens), 0)
        < lax.broadcasted_iota(jnp.int32, (tokens, tokens), 1)
    ).astype(F32)
    rank = jnp.dot(sum(hots), earlier, preferred_element_type=F32)
    where = rank + (expert * slots).astype(F32)
    slot = lax.broadcasted_iota(jnp.int32, (experts * slots, tokens), 0).astype(F32)
    return [
        (slot == jnp.sum(hot * where, axis=0, keepdims=True)).astype(F32) for hot in hots
    ]


def attend_kernel(
    n, slots,
    blk_ref, qn_ref, qr_ref, cos_ref, sin_ref, upk_ref, upv_ref, ow_ref, res_ref, gain_ref,
    picks_ref, mid_ref, out_ref, rows, qrot, att, norm, send_sem, recv_sem,
):
    tokens = blk_ref.shape[0]
    width = res_ref.shape[1]
    me = lax.axis_index("sp")
    barrier = pltpu.get_barrier_semaphore()
    for d in range(1, n):
        pl.semaphore_signal(
            barrier, inc=1, device_id={"sp": lax.rem(me + d, n)}, device_id_type=MESH
        )
    pl.semaphore_wait(barrier, n - 1)
    copies = []
    for d in range(1, n):
        copy = pltpu.make_async_remote_copy(
            src_ref=blk_ref,
            dst_ref=rows.at[pl.ds(d * tokens, tokens)],
            send_sem=send_sem.at[d],
            recv_sem=recv_sem.at[d],
            device_id={"sp": lax.rem(me + d, n)},
            device_id_type=MESH,
        )
        copy.start()
        copies.append(copy)
    rows[:tokens, :] = blk_ref[...]
    for g in range(HEADS * ROPE // LANES):
        x = qr_ref[:, g * LANES : (g + 1) * LANES].astype(F32)
        qrot[:, g * LANES : (g + 1) * LANES] = (
            x * cos_ref[...] + swapped(x) * sin_ref[...]
        ).astype(BF16)
    factor = (NOPE + ROPE) ** (-0.5)
    lane = lax.broadcasted_iota(jnp.int32, (tokens, LANES), 1)
    low = lane < NOPE
    lowb = low.astype(F32).astype(BF16)
    highb = (lane >= NOPE).astype(F32).astype(BF16)
    ropeb = [(lane // ROPE == k).astype(F32).astype(BF16) for k in range(LANES // ROPE)]
    for copy in copies:
        copy.wait()

    def group(g, carry):
        turned = qrot[:, pl.ds(pl.multiple_of(g * LANES, LANES), LANES)]
        for q in range(2):
            lanes = pl.ds(pl.multiple_of((g * 2 + q) * LANES, LANES), LANES)
            lat = rows[:, :LATENT]
            keys = jnp.dot(lat, upk_ref[:, lanes], preferred_element_type=F32).astype(BF16)
            vals = jnp.dot(lat, upv_ref[:, lanes], preferred_element_type=F32).astype(BF16)
            keys = jnp.concatenate([keys, rows[:, LATENT:]], axis=1)
            plain = qn_ref[:, lanes]
            first = jnp.concatenate([plain * lowb, turned * ropeb[2 * q]], axis=1)
            second = jnp.concatenate([plain * highb, turned * ropeb[2 * q + 1]], axis=1)
            query = jnp.concatenate([first, second], axis=0)
            scores = lax.dot_general(
                query, keys, (((1,), (1,)), ((), ())), preferred_element_type=F32
            ) * factor
            weights = jnp.exp(scores - jnp.max(scores, axis=-1, keepdims=True))
            total = jnp.sum(weights, axis=-1, keepdims=True)
            mixed = jnp.dot(weights.astype(BF16), vals, preferred_element_type=F32) / total
            att[:, lanes] = jnp.where(low, mixed[:tokens], mixed[tokens:]).astype(BF16)
        return carry

    lax.fori_loop(0, HEADS * ROPE // LANES, group, 0)
    step = 512

    def project(c, square):
        cols = pl.ds(pl.multiple_of(c * step, step), step)
        product = jnp.dot(att[...], ow_ref[:, cols], preferred_element_type=F32)
        middle = (res_ref[:, cols].astype(F32) + product).astype(BF16)
        mid_ref[:, cols] = middle
        wide = middle.astype(F32)
        return square + jnp.sum(wide * wide, axis=-1, keepdims=True)

    square = lax.fori_loop(0, width // step, project, jnp.zeros((tokens, 1), F32))
    scale = lax.rsqrt(square / width + EPS)
    norm[...] = (mid_ref[...].astype(F32) * scale * gain_ref[...]).astype(BF16)
    packer = sum(place(picks_ref, n, slots, tokens)).astype(BF16)

    def pack(c, carry):
        cols = pl.ds(pl.multiple_of(c * step, step), step)
        out_ref[:, cols] = jnp.dot(packer, norm[:, cols], preferred_element_type=F32).astype(BF16)
        return carry

    lax.fori_loop(0, width // step, pack, 0)


def expert_kernel(
    n, m, slots,
    sent_ref, gate_ref, up_ref, down_ref, mid_ref, picks_ref, weight_ref, out_ref,
    held, red, fin, back, local_sem, send_sem, recv_sem,
):
    tokens, width = mid_ref.shape
    groups = m // 2
    me = lax.axis_index("sp")
    rank = lax.axis_index("tp")
    sibling = rank + 1 - 2 * lax.rem(rank, 2)
    parts = min(4, n)
    count = n // parts
    span = count * slots
    step = 512
    barrier = pltpu.get_barrier_semaphore()
    for d in range(1, n):
        pl.semaphore_signal(
            barrier, inc=1, device_id={"sp": lax.rem(me + d, n)}, device_id_type=MESH
        )
    for j in range(1, groups):
        pl.semaphore_signal(
            barrier, inc=1, device_id={"tp": lax.rem(rank + 2 * j, m)}, device_id_type=MESH
        )
    pl.semaphore_signal(barrier, inc=1, device_id={"tp": sibling}, device_id_type=MESH)
    pl.semaphore_wait(barrier, n + groups - 1)
    used = [0]

    def remote(source, target, device):
        index = used[0]
        used[0] += 1
        copy = pltpu.make_async_remote_copy(
            src_ref=source,
            dst_ref=target,
            send_sem=send_sem.at[index],
            recv_sem=recv_sem.at[index],
            device_id=device,
            device_id_type=MESH,
        )
        copy.start()
        return copy

    first = pltpu.make_async_copy(
        sent_ref.at[pl.ds(me * slots, slots)], held.at[0, 0, pl.ds(0, slots)], local_sem
    )
    first.start()
    arrive = [first]
    for d in range(1, n):
        peer = lax.rem(me + d, n)
        arrive.append(
            remote(
                sent_ref.at[pl.ds(peer * slots, slots)],
                held.at[0, 0, pl.ds(d * slots, slots)],
                {"sp": peer},
            )
        )
    across, aside, reduced, final, returned = {}, {}, {}, {}, {}

    def forward(k):
        rows = pl.ds(k * span, span)
        for d in range(k * count, (k + 1) * count):
            arrive[d].wait()
        for j in range(1, groups):
            across[k, j] = remote(
                held.at[0, 0, rows], held.at[j, 0, rows], {"tp": lax.rem(rank + 2 * j, m)}
            )
        aside[k, 0] = remote(held.at[0, 0, rows], held.at[0, 1, rows], {"tp": sibling})

    def relay(k):
        rows = pl.ds(k * span, span)
        for j in range(1, groups):
            across[k, j].wait()
            aside[k, j] = remote(held.at[j, 0, rows], held.at[j, 1, rows], {"tp": sibling})

    def compute(k):
        rows = pl.ds(k * span, span)
        for j in range(groups):
            aside[k, j].wait()
        block = jnp.concatenate(
            [held[j, c, rows, :] for j in range(groups) for c in range(2)], axis=0
        )
        gate = jnp.minimum(jnp.dot(block, gate_ref[...], preferred_element_type=F32), CLAMP)
        lift = jnp.clip(
            jnp.dot(block, up_ref[...], preferred_element_type=F32), -CLAMP, CLAMP
        )
        active = (gate * jax.nn.sigmoid(ALPHA * gate) * (lift + 1.0)).astype(BF16)

        def down(c, carry):
            cols = pl.ds(pl.multiple_of(c * step, step), step)
            term = jnp.dot(active, down_ref[:, cols], preferred_element_type=F32).astype(BF16)
            for i in range(m):
                held[i // 2, i % 2, rows, cols] = term[i * span : (i + 1) * span]
            return carry

        lax.fori_loop(0, width // step, down, 0)
        for j in range(groups):
            reduced[k, j] = remote(held.at[j, 1, rows], red.at[j, rows], {"tp": sibling})

    def reduce(k):
        rows = pl.ds(k * span, span)
        for j in list(range(1, groups)) + [0]:
            reduced[k, j].wait()
            total = held[j, 0, rows, :].astype(F32) + red[j, rows, :].astype(F32)
            held[j, 0, rows, :] = total.astype(BF16)
            if j:
                final[k, j] = remote(
                    held.at[j, 0, rows], fin.at[j - 1, rows], {"tp": lax.rem(rank + m - 2 * j, m)}
                )

    def finish(k):
        rows = pl.ds(k * span, span)
        total = held[0, 0, rows, :].astype(F32)
        for j in range(1, groups):
            final[k, j].wait()
            total = total + fin[j - 1, rows, :].astype(F32)
        held[0, 0, rows, :] = total.astype(BF16)
        for d in range(k * count, (k + 1) * count):
            source = held.at[0, 0, pl.ds(d * slots, slots)]
            target = back.at[pl.ds(me * slots, slots)]
            if d:
                returned[d] = remote(source, target, {"sp": lax.rem(me + n - d, n)})
            else:
                returned[d] = pltpu.make_async_copy(source, target, local_sem)
                returned[d].start()

    for t in range(parts + 4):
        for work, k in ((forward, t), (relay, t - 1), (compute, t - 2), (reduce, t - 3), (finish, t - 4)):
            if 0 <= k < parts:
                work(k)
    spots = place(picks_ref, n, slots, tokens)
    high = low = 0.0
    for k in range(TOPK):
        weight = weight_ref[k : k + 1, :]
        coarse = weight.astype(BF16).astype(F32)
        high = high + spots[k] * coarse
        low = low + spots[k] * (weight - coarse)
    high = high.astype(BF16)
    low = low.astype(BF16)
    dims = (((0,), (0,)), ((), ()))
    for d in range(n):
        returned[d].wait()

    def chunk(c, carry):
        cols = pl.ds(pl.multiple_of(c * step, step), step)
        rows = back[:, cols]
        added = lax.dot_general(high, rows, dims, preferred_element_type=F32)
        added = added + lax.dot_general(low, rows, dims, preferred_element_type=F32)
        out_ref[:, cols] = (mid_ref[:, cols].astype(F32) + added).astype(BF16)
        return carry

    lax.fori_loop(0, width // step, chunk, 0)


def local(
    residual, query_nope, query_rope, latent, rope_key, latent_gain, up_key, up_value,
    out_weight, ffn_gain, routes, route_weight, gate_weight, up_weight, down_weight,
):
    tokens, width = residual.shape[1:]
    n = lax.axis_size("sp")
    slots = min(tokens, max(2, 5 * tokens * TOPK // (4 * n)))
    slots = -(-slots // 16) * 16
    positions = lax.axis_index("sp") * tokens + jnp.arange(tokens, dtype=jnp.int32)
    lane = jnp.arange(LANES, dtype=jnp.int32)
    half = ROPE // 2
    inverse = ROPE_BASE ** (-(lane % half).astype(F32) * 2.0 / ROPE)
    angle = positions.astype(F32)[:, None] * inverse[None, :]
    cosine = jnp.cos(angle)
    sine = jnp.sin(angle) * jnp.where(lane % ROPE < half, -1.0, 1.0)[None, :]
    blk = pl.pallas_call(
        prep_kernel,
        out_shape=jax.ShapeDtypeStruct((tokens, 2 * LANES), BF16),
        in_specs=[VM] * 5,
        out_specs=VM,
    )(latent[0], latent_gain[None, :], jnp.tile(rope_key[0], (1, LANES // ROPE)), cosine, sine)
    picks = lax.dynamic_index_in_dim(
        jnp.transpose(routes, (0, 2, 1)), lax.axis_index("tp"), 0, keepdims=False
    )
    middle, outgoing = pl.pallas_call(
        functools.partial(attend_kernel, n, slots),
        out_shape=(
            jax.ShapeDtypeStruct((tokens, width), BF16),
            jax.ShapeDtypeStruct((n * slots, width), BF16),
        ),
        in_specs=[VM] * 11,
        out_specs=(VM, VM),
        scratch_shapes=[
            pltpu.VMEM((n * tokens, 2 * LANES), BF16),
            pltpu.VMEM((tokens, HEADS * ROPE), BF16),
            pltpu.VMEM((tokens, HEADS * VDIM), BF16),
            pltpu.VMEM((tokens, width), BF16),
            pltpu.SemaphoreType.DMA((n,)),
            pltpu.SemaphoreType.DMA((n,)),
        ],
        compiler_params=pltpu.CompilerParams(
            collective_id=0, has_side_effects=True, vmem_limit_bytes=60 * 2**20
        ),
    )(
        blk, query_nope[0], query_rope[0], cosine, sine, up_key, up_value, out_weight,
        residual[0], ffn_gain[None, :], picks,
    )
    m = lax.axis_size("tp")
    copies = 2 * (n - 1) + min(4, n) * (4 * (m // 2) - 2)
    updated = pl.pallas_call(
        functools.partial(expert_kernel, n, m, slots),
        out_shape=jax.ShapeDtypeStruct((tokens, width), BF16),
        in_specs=[VM] * 7,
        out_specs=VM,
        scratch_shapes=[
            pltpu.VMEM((m // 2, 2, n * slots, width), BF16),
            pltpu.VMEM((m // 2, n * slots, width), BF16),
            pltpu.VMEM((max(1, m // 2 - 1), n * slots, width), BF16),
            pltpu.VMEM((n * slots, width), BF16),
            pltpu.SemaphoreType.DMA,
            pltpu.SemaphoreType.DMA((copies,)),
            pltpu.SemaphoreType.DMA((copies,)),
        ],
        compiler_params=pltpu.CompilerParams(
            collective_id=1, has_side_effects=True, vmem_limit_bytes=60 * 2**20
        ),
    )(
        outgoing, gate_weight[0], up_weight[0], down_weight[0], middle, picks,
        jnp.transpose(route_weight[0], (1, 0)),
    )
    return updated[None]


def solution(mesh):
    in_specs = (
        P("tp", "sp", None),
        P("tp", "sp", None),
        P("tp", "sp", None),
        P("tp", "sp", None),
        P("tp", "sp", None),
        P(),
        P(),
        P(),
        P(),
        P(),
        P(None, "sp", None),
        P("tp", "sp", None),
        P("sp", None, "tp"),
        P("sp", None, "tp"),
        P("sp", "tp", None),
    )
    out_specs = P("tp", "sp", None)
    return jax.shard_map(local, mesh=mesh, in_specs=in_specs, out_specs=out_specs, check_vma=False)
```
